32 devices in a mesh: grp: 2 (over x), ra: 4 (over z), cb: 4 (over y, core).
Axes of the slice: x: 2, y: 2, z: 4, core: 2. Of those that a mesh axis runs over, the one named last changes fastest.
Arguments:
- tokens: bfloat16 [256, 4096], P('grp', 'ra'), parts along dimension 0, may hold values from -30 to 30
- in_gain: float32 [4096], P('ra'), may hold values from 0.1 to 1.9
- gate_weight: float32 [4096, 11264], P('ra', 'cb'), may hold values from -0.09375 to 0.09375
- gate_scale: float32 [11264], P('cb'), may hold values from 0.3 to 3
- up_weight: float32 [4096, 11264], P('ra', 'cb'), may hold values from -0.09375 to 0.09375
- up_scale: float32 [11264], P('cb'), may hold values from 0.3 to 3
- down_weight: float32 [11264, 4096], P('cb', 'ra'), may hold values from -0.0546875 to 0.0546875
- down_scale: float32 [4096], P('ra'), may hold values from 0.3 to 3
- out_gain: float32 [4096], P('ra'), may hold values from 0.1 to 1.9
Outputs:
- result: bfloat16 [256, 4096], P('grp', 'ra'), parts along dimension 0
The draws below stay inside these ranges and needn't reach their ends.
There are 2 independent parts, one for each index of `grp`. The reference program is written for one: setup_inputs(seed, part) draws one part's arguments, and reference() takes and returns one part's arrays. A program takes and returns all parts, laid end to end along the dimension named above; an argument that names none is the same for every part. Nothing has to cross between parts.
All inputs are finite; a program needn't handle non-finite values.
Results may differ from the reference program's by a relative error of at most 0.008.
Values may be sent and summed in bfloat16 or wider, within the bound.
No kernel may reach another device: no remote copies, remote signals or barrier semaphores. Data moves between devices by JAX's collectives and lax.ppermute only.
A program may use at most 64 MiB of HBM per device.

```python
import math
import jax
import jax.numpy as jnp
from jax import lax

D = 4096
FF = 11264
TOK = 128


def draw_tokens(key, part):
    keys = jax.random.split(jax.random.fold_in(key, 11), 2)
    column = jnp.exp(math.log(10.0) * jnp.arange(D, dtype=jnp.float32) / (D - 1))
    rows = jnp.exp(jax.random.uniform(keys[0], (TOK, 1), jnp.float32, 0.0, math.log(10.0)))
    base = jax.random.normal(keys[1], (TOK, D), jnp.float32)
    values = base * rows * column[None, :]
    values = values / jnp.sqrt(jnp.mean(values * values))
    return jnp.clip(values, -30.0, 30.0).astype(jnp.bfloat16)


def levels(key, dims, cuts, low, high):
    gain, own = 1.0, jax.random.fold_in(key, 6)
    for axis_at, blocks in cuts:
        draws = jnp.exp(jax.random.uniform(jax.random.fold_in(own, axis_at), (blocks,), jnp.float32, low / len(cuts), high / len(cuts)))
        gain = gain * jnp.repeat(draws, dims[axis_at] // blocks).reshape([-1 if axis == axis_at else 1 for axis in range(len(dims))])
    return gain


def bell_draw(rng, extent, spread, most, pieces=(), kind=jnp.bfloat16):
    gain = levels(rng, extent, pieces, -0.22, 0.18) if pieces else 1.0
    drawn = jax.random.normal(rng, extent, jnp.float32) * spread * gain
    return jnp.minimum(jnp.maximum(drawn, -most), most).astype(kind)


def setup_inputs(seed: int = 0, part: int = 0) -> dict:
    arg_keys = jax.random.split(jax.random.key(seed), 10)
    own_keys = jax.random.split(jax.random.fold_in(arg_keys[9], part), 10)
    return {
        "tokens": draw_tokens(jax.random.fold_in(jax.random.fold_in(arg_keys[9], part), 71), part),
        "in_gain": jnp.clip(1.0 + 0.18 * jax.random.normal(arg_keys[1], (D,), jnp.float32), 0.1, 1.9),
        "gate_weight": bell_draw(arg_keys[2], (D, FF), D ** -0.5, 0.09375, ((0, 4), (1, 4)), jnp.float32),
        "gate_scale": jnp.clip(jnp.exp(math.log(3.0) - 2.3025851 * jax.random.uniform(arg_keys[3], (FF,), jnp.float32) ** levels(arg_keys[3], (FF,), ((0, 4),), -0.2, 0.2)), 0.3, 3.0),
        "up_weight": bell_draw(arg_keys[4], (D, FF), D ** -0.5, 0.09375, ((0, 4), (1, 4)), jnp.float32),
        "up_scale": jnp.clip(jnp.exp(math.log(3.0) - 2.3025851 * jax.random.uniform(arg_keys[5], (FF,), jnp.float32) ** levels(arg_keys[5], (FF,), ((0, 4),), -0.2, 0.2)), 0.3, 3.0),
        "down_weight": bell_draw(arg_keys[6], (FF, D), FF ** -0.5, 0.0546875, ((0, 4), (1, 4)), jnp.float32),
        "down_scale": jnp.clip(jnp.exp(math.log(3.0) - 2.3025851 * jax.random.uniform(arg_keys[7], (D,), jnp.float32) ** levels(arg_keys[7], (D,), ((0, 4),), -0.2, 0.2)), 0.3, 3.0),
        "out_gain": jnp.clip(1.0 + 0.18 * jax.random.normal(arg_keys[8], (D,), jnp.float32), 0.1, 1.9),
    }


EPSILON = 1e-06
RESIDUAL = 0.5

def reference(tokens, in_gain, gate_weight, gate_scale, up_weight, up_scale, down_weight, down_scale, out_gain):
    tok_float = tokens.astype(jnp.float32)
    inv_rows = lax.rsqrt(lax.optimization_barrier(jnp.mean(tok_float * tok_float, axis=1, keepdims=True)) + EPSILON)
    scaled = (tok_float * in_gain[None, :]).astype(jnp.bfloat16)
    gate_full = jnp.dot(scaled, gate_weight.astype(jnp.bfloat16), preferred_element_type=jnp.float32) * inv_rows * gate_scale[None, :]
    up_full = jnp.dot(scaled, up_weight.astype(jnp.bfloat16), preferred_element_type=jnp.float32) * inv_rows * up_scale[None, :]
    hidden = (jax.nn.silu(gate_full) * up_full).astype(jnp.bfloat16)
    down_full = jnp.dot(hidden, down_weight.astype(jnp.bfloat16), preferred_element_type=jnp.float32)
    mixed_rows = RESIDUAL * tok_float + down_full * down_scale[None, :]
    inv_out = lax.rsqrt(lax.optimization_barrier(jnp.mean(mixed_rows * mixed_rows, axis=1, keepdims=True)) + EPSILON)
    return (mixed_rows * inv_out * out_gain[None, :]).astype(jnp.bfloat16)
```

```python
import jax
import jax.numpy as jnp
from jax import lax
from jax.sharding import PartitionSpec as P

EPSILON = 1e-06
RESIDUAL = 0.5
LANES = 128
CHUNKS = (7, 15)


def column_chunks(columns):
    if columns % (LANES * sum(CHUNKS)):
        return [(0, columns)]
    unit, ranges, start = columns // sum(CHUNKS), [], 0
    for size in CHUNKS:
        ranges.append((start, start + size * unit))
        start += size * unit
    return ranges


def roll_blocks(blocks, shift):
    count = blocks.shape[0]
    twice = jnp.concatenate([blocks, blocks], axis=0)
    return lax.dynamic_slice_in_dim(twice, (count - shift) % count, count, axis=0)


def local(
    tokens, in_gain, gate_weight, gate_scale, up_weight, up_scale, down_weight, down_scale, out_gain
):
    f32, bf16 = jnp.float32, jnp.bfloat16
    ra, cb = lax.axis_size("ra"), lax.axis_size("cb")
    z, c = lax.axis_index("ra"), lax.axis_index("cb")
    rows, width = tokens.shape
    share, features = rows // ra, width * ra
    half = rows // 2

    def send(x, step):
        return lax.ppermute(x, "ra", [(i, (i + step) % ra) for i in range(ra)])

    def swap(x, bit):
        return lax.ppermute(x, "cb", [(i, i ^ bit) for i in range(cb)])

    def share_of(x, at):
        return lax.dynamic_index_in_dim(x.reshape(ra, share, *x.shape[1:]), at % ra, 0, False)

    tok_float = tokens.astype(f32)
    scaled = (tok_float * in_gain[None, :]).astype(bf16)
    squares = jnp.sum(tok_float * tok_float, axis=1)
    own_squares = share_of(squares, z)
    for step in range(1, ra):
        own_squares = own_squares + send(share_of(squares, z + step), step)
    inv_rows = lax.rsqrt(own_squares / features + EPSILON)[:, None]

    ranges = column_chunks(gate_weight.shape[1])
    sums = []
    for lo, hi in ranges:
        gate_part = jnp.dot(scaled, gate_weight[:, lo:hi].astype(bf16), preferred_element_type=f32)
        up_part = jnp.dot(scaled, up_weight[:, lo:hi].astype(bf16), preferred_element_type=f32)
        both = jnp.concatenate([gate_part.astype(bf16), up_part.astype(bf16)], axis=1)
        gate_sum, up_sum = share_of(gate_part, z), share_of(up_part, z)
        for step in range(1, ra):
            got = send(share_of(both, z + step), step).astype(f32)
            gate_sum, up_sum = gate_sum + got[:, : hi - lo], up_sum + got[:, hi - lo :]
        sums.append((gate_sum, up_sum))

    down_bf16 = lax.optimization_barrier(down_weight.astype(bf16))
    down_part = jnp.zeros((rows, width), f32)
    for (lo, hi), (gate_sum, up_sum) in zip(ranges, sums):
        gate_share = gate_sum * inv_rows * gate_scale[None, lo:hi]
        up_share = up_sum * inv_rows * up_scale[None, lo:hi]
        hidden = (jax.nn.silu(gate_share) * up_share).astype(bf16)
        blocks = [hidden] + [send(hidden, ra - step) for step in range(1, ra)]
        down_part = down_part + jnp.dot(
            jnp.concatenate(blocks, axis=0), down_bf16[lo:hi], preferred_element_type=f32
        )

    core = c % 2
    pair = down_part.reshape(2, half, width)
    mine = lax.dynamic_index_in_dim(pair, core, 0, False)
    other = lax.dynamic_index_in_dim(pair, 1 - core, 0, False)
    summed = mine + swap(other, 1)
    bit = 2
    while bit < cb:
        rounded = lax.reduce_precision(summed, 8, 7)
        summed = rounded + swap(rounded.astype(bf16), bit).astype(f32)
        bit *= 2
    turned = roll_blocks(tokens.reshape(ra, share, width), (ra - z) % ra).reshape(2, half, width)
    residual = lax.dynamic_index_in_dim(turned, core, 0, False).astype(f32)
    mixed_half = RESIDUAL * residual + summed * down_scale[None, :]
    mixed = jnp.stack([mixed_half, swap(mixed_half, 1)]).reshape(ra, share, width)
    mixed = roll_blocks(mixed, (z + core * (ra // 2)) % ra).reshape(rows, width)
    out_squares = jnp.sum(mixed * mixed, axis=1)
    total = out_squares
    for step in range(1, ra):
        total = total + send(out_squares, step)
    inv_out = lax.rsqrt(total / features + EPSILON)[:, None]
    return (mixed * inv_out * out_gain[None, :]).astype(bf16)


def solution(mesh):
    in_specs = (
        P("grp", "ra"),
        P("ra"),
        P("ra", "cb"),
        P("cb"),
        P("ra", "cb"),
        P("cb"),
        P("cb", "ra"),
        P("ra"),
        P("ra"),
    )
    out_specs = P("grp", "ra")
    return jax.shard_map(local, mesh=mesh, in_specs=in_specs, out_specs=out_specs, check_vma=False)
```

```python
import jax
import jax.numpy as jnp
from jax import lax
from jax.experimental import pallas as pl
from jax.experimental.pallas import tpu as pltpu
from jax.sharding import PartitionSpec as P

EPSILON = 1e-06
RESIDUAL = 0.5
TILE = 256
CHUNKS = (3, 4, 4)


def column_chunks(columns):
    if columns % (TILE * sum(CHUNKS)):
        return columns, [(0, 1)]
    unit, ranges, start = columns // (TILE * sum(CHUNKS)), [], 0
    for size in CHUNKS:
        ranges.append((start, start + size * unit))
        start += size * unit
    return TILE, ranges


def partial_products(tokens, in_gain, gate_weight, up_weight, z, tile, lo, hi):
    ra, share, width = tokens.shape
    f32, bf16 = jnp.float32, jnp.bfloat16

    def kernel(z_ref, tok_ref, gain_ref, gate_ref, up_ref, own_ref, *rest):
        sends, scaled = rest[:-1], rest[-1]

        @pl.when(pl.program_id(0) == 0)
        def _():
            for j in range(ra):
                block = tok_ref[lax.rem(z_ref[0] + j, ra)].astype(f32) * gain_ref[...]
                scaled[j * share : (j + 1) * share] = block.astype(bf16)

        for i, weight in enumerate((gate_ref, up_ref)):
            part = jnp.dot(scaled[...], weight[...].astype(bf16), preferred_element_type=f32)
            own_ref[i] = part[:share]
            for j, out in enumerate(sends):
                out[i] = part[(j + 1) * share : (j + 2) * share].astype(bf16)

    columns = (hi - lo) * tile
    weight_spec = pl.BlockSpec((width, tile), lambda t: (0, t + lo))
    out_spec = pl.BlockSpec((2, share, tile), lambda t: (0, 0, t))
    shapes = [jax.ShapeDtypeStruct((2, share, columns), f32)]
    shapes += [jax.ShapeDtypeStruct((2, share, columns), bf16)] * (ra - 1)
    return pl.pallas_call(
        kernel,
        grid=(hi - lo,),
        in_specs=[
            pl.BlockSpec(memory_space=pltpu.SMEM),
            pl.BlockSpec((ra, share, width), lambda t: (0, 0, 0)),
            pl.BlockSpec((1, width), lambda t: (0, 0)),
            weight_spec,
            weight_spec,
        ],
        out_specs=[out_spec] * ra,
        out_shape=shapes,
        scratch_shapes=[pltpu.VMEM((ra * share, width), bf16)],
        compiler_params=pltpu.CompilerParams(dimension_semantics=("arbitrary",)),
    )(z.reshape(1), tokens, in_gain.reshape(1, width), gate_weight, up_weight)


def roll_blocks(blocks, shift):
    count = blocks.shape[0]
    twice = jnp.concatenate([blocks, blocks], axis=0)
    return lax.dynamic_slice_in_dim(twice, (count - shift) % count, count, axis=0)


def local(
    tokens, in_gain, gate_weight, gate_scale, up_weight, up_scale, down_weight, down_scale, out_gain
):
    f32, bf16 = jnp.float32, jnp.bfloat16
    ra, cb = lax.axis_size("ra"), lax.axis_size("cb")
    z, c = lax.axis_index("ra"), lax.axis_index("cb")
    rows, width = tokens.shape
    share, features = rows // ra, width * ra
    half = rows // 2

    def send(x, step):
        return lax.ppermute(x, "ra", [(i, (i + step) % ra) for i in range(ra)])

    def swap(x, bit):
        return lax.ppermute(x, "cb", [(i, i ^ bit) for i in range(cb)])

    def share_of(x, at):
        return lax.dynamic_index_in_dim(x.reshape(ra, share, *x.shape[1:]), at % ra, 0, False)

    blocks3 = tokens.reshape(ra, share, width)
    tile, ranges = column_chunks(gate_weight.shape[1])
    sums, inv_rows = [], None
    for lo, hi in ranges:
        own, *outgoing = partial_products(
            blocks3, in_gain, gate_weight, up_weight, z, tile, lo, hi
        )
        received = [send(x, step + 1) for step, x in enumerate(outgoing)]
        sums.append((own, received))
        if inv_rows is None:
            tok_after, _ = lax.optimization_barrier((tokens, own))
            tok_float = tok_after.astype(f32)
            squares = jnp.sum(tok_float * tok_float, axis=1)
            own_squares = share_of(squares, z)
            for step in range(1, ra):
                own_squares = own_squares + send(share_of(squares, z + step), step)
            inv_rows = lax.rsqrt(own_squares / features + EPSILON)[:, None]

    down_after, _ = lax.optimization_barrier((down_weight, sums[-1][0]))
    down_bf16 = lax.optimization_barrier(down_after.astype(bf16))
    down_part = jnp.zeros((rows, width), f32)
    hidden = None
    for (lo, hi), (own, received) in zip(ranges, sums):
        lo, hi = lo * tile, hi * tile
        if hidden is not None:
            received, _ = lax.optimization_barrier((received, hidden))
        total = own
        for got in received:
            total = total + got.astype(f32)
        gate_share = total[0] * inv_rows * gate_scale[None, lo:hi]
        up_share = total[1] * inv_rows * up_scale[None, lo:hi]
        hidden = (jax.nn.silu(gate_share) * up_share).astype(bf16)
        blocks = [hidden] + [send(hidden, ra - step) for step in range(1, ra)]
        down_part = down_part + jnp.dot(
            jnp.concatenate(blocks, axis=0), down_bf16[lo:hi], preferred_element_type=f32
        )

    core = c % 2
    pair = down_part.reshape(2, half, width)
    mine = lax.dynamic_index_in_dim(pair, core, 0, False)
    other = lax.dynamic_index_in_dim(pair, 1 - core, 0, False)
    summed = mine + swap(other, 1)
    bit = 2
    while bit < cb:
        rounded = lax.reduce_precision(summed, 8, 7)
        summed = rounded + swap(rounded.astype(bf16), bit).astype(f32)
        bit *= 2
    turned = roll_blocks(tokens.reshape(ra, share, width), (ra - z) % ra).reshape(2, half, width)
    residual = lax.dynamic_index_in_dim(turned, core, 0, False).astype(f32)
    mixed_half = RESIDUAL * residual + summed * down_scale[None, :]
    mixed = jnp.stack([mixed_half, swap(mixed_half, 1)]).reshape(ra, share, width)
    mixed = roll_blocks(mixed, (z + core * (ra // 2)) % ra).reshape(rows, width)
    out_squares = jnp.sum(mixed * mixed, axis=1)
    total = out_squares
    for step in range(1, ra):
        total = total + send(out_squares, step)
    inv_out = lax.rsqrt(total / features + EPSILON)[:, None]
    return (mixed * inv_out * out_gain[None, :]).astype(bf16)


def solution(mesh):
    in_specs = (
        P("grp", "ra"),
        P("ra"),
        P("ra", "cb"),
        P("cb"),
        P("ra", "cb"),
        P("cb"),
        P("cb", "ra"),
        P("ra"),
        P("ra"),
    )
    out_specs = P("grp", "ra")
    return jax.shard_map(local, mesh=mesh, in_specs=in_specs, out_specs=out_specs, check_vma=False)
```
